32 devices in a mesh: grp: 2 (over y), fs: 4 (over z), tp: 4 (over x, core).
Axes of the slice: x: 2, y: 2, z: 4, core: 2. Of those that a mesh axis runs over, the one named last changes fastest.
Arguments:
- tokens: bfloat16 [2048, 2048], P(('grp', 'fs', 'tp')), parts along dimension 0, may hold values from -30 to 30
- gate_master: float32 [2048, 2752], P('fs', 'tp'), may hold values from -0.125 to 0.125
- up_master: float32 [2048, 2752], P('fs', 'tp'), may hold values from -0.125 to 0.125
- down_master: float32 [2048, 2752], P('fs', 'tp'), may hold values from -0.4375 to 0.4375
- norm_gain: float32 [2048], replicated, may hold values from 0.1 to 1.9
- post_gain: float32 [2048], replicated, may hold values from 0.1 to 1.9
- post_bias: float32 [2048], replicated, may hold values from -3 to 3
Outputs:
- gate_ready: bfloat16 [4096, 2752], P('grp', 'tp'), parts along dimension 0
- up_ready: bfloat16 [4096, 2752], P('grp', 'tp'), parts along dimension 0
- down_ready: bfloat16 [4096, 2752], P('grp', 'tp'), parts along dimension 0
- result: bfloat16 [2048, 2048], P(('grp', 'fs', 'tp')), parts along dimension 0
The draws below stay inside these ranges and needn't reach their ends.
There are 2 independent parts, one for each index of `grp`. The reference program is written for one: setup_inputs(seed, part) draws one part's arguments, and reference() takes and returns one part's arrays. A program takes and returns all parts, laid end to end along the dimension named above; an argument that names none is the same for every part. Nothing has to cross between parts.
All inputs are finite; a program needn't handle non-finite values.
Results may differ from the reference program's by a relative error of at most 0.009.
Values may be sent and summed in bfloat16 or wider, within the bound.
A program may use at most 64 MiB of HBM per device.

```python
import math
import jax
import jax.numpy as jnp
from jax import lax

D = 2048
FF = 2752
TOKENS = 1024
N_TP = 4


def draw_tokens(key, part):
    key_base, key_rows, key_cols = jax.random.split(key, 3)
    row_scale = jnp.exp(jax.random.uniform(key_rows, (TOKENS, 1), jnp.float32, math.log(0.3), math.log(3.0)))
    col_scale = jnp.exp(jax.random.uniform(key_cols, (1, D), jnp.float32, math.log(0.5), math.log(2.0)))
    base = jnp.clip(jax.random.normal(key_base, (TOKENS, D), jnp.float32), -4.0, 4.0)
    return (base * row_scale * col_scale).astype(jnp.bfloat16)


def shard_levels(rng, dims, pieces, least, top_value):
    gain = 1.0
    for axis_at, parts in pieces:
        draws = jax.random.uniform(jax.random.fold_in(jax.random.fold_in(rng, 6), axis_at), (parts,), jnp.float32, least / len(pieces), top_value / len(pieces))
        gain = gain * jnp.repeat(jnp.exp(draws), dims[axis_at] // parts).reshape((-1,) + (1,) * (len(dims) - 1 - axis_at))
    return gain


def centred(key, shape, deviation, most, cuts=(), kind=jnp.bfloat16):
    values = deviation * jax.random.normal(key, shape, jnp.float32)
    if cuts:
        values = values * shard_levels(key, shape, cuts, -0.22, 0.18)
    return jnp.clip(values, -most, most).astype(kind)


def setup_inputs(seed: int = 0, part: int = 0) -> dict:
    streams_of = jax.random.split(jax.random.key(seed), 8)
    part_keys = jax.random.split(jax.random.fold_in(streams_of[7], part), 8)
    return {
        "tokens": draw_tokens(jax.random.fold_in(jax.random.fold_in(streams_of[7], part), 71), part),
        "gate_master": centred(streams_of[1], (D, FF), D ** -0.5, 0.125, ((0, 4), (1, 4)), jnp.float32),
        "up_master": centred(streams_of[2], (D, FF), D ** -0.5, 0.125, ((0, 4), (1, 4)), jnp.float32),
        "down_master": centred(streams_of[3], (D, FF), (FF // 16) ** -0.5, 0.4375, ((0, 4), (1, 4)), jnp.float32),
        "norm_gain": jnp.clip(1.0 + 0.18 * jax.random.normal(streams_of[4], (D,), jnp.float32), 0.1, 1.9),
        "post_gain": jnp.clip(1.0 + 0.18 * jax.random.normal(streams_of[5], (D,), jnp.float32), 0.1, 1.9),
        "post_bias": centred(streams_of[6], (D,), 0.5, 3.0, (), jnp.float32),
    }


def reference(tokens, gate_master, up_master, down_master, norm_gain, post_gain, post_bias):
    gate_ready = (norm_gain[:, None] * gate_master).astype(jnp.bfloat16)
    up_ready = (norm_gain[:, None] * up_master).astype(jnp.bfloat16)
    down_ready = down_master.astype(jnp.bfloat16)
    wide = tokens.astype(jnp.float32)
    normed = (wide * lax.rsqrt(lax.optimization_barrier(jnp.mean(wide * wide, axis=-1, keepdims=True)) + 1e-06)).astype(jnp.bfloat16)
    gate = jnp.dot(normed, gate_ready, preferred_element_type=jnp.float32)
    upward = jnp.dot(normed, up_ready, preferred_element_type=jnp.float32)
    hidden = (jax.nn.silu(gate) * upward).astype(jnp.bfloat16)
    block_units = FF // N_TP
    branch = jnp.zeros((tokens.shape[0], D), jnp.float32)
    for block in range(N_TP):
        part_hidden = hidden[:, block * block_units:(block + 1) * block_units]
        part_down = down_ready[:, block * block_units:(block + 1) * block_units]
        partial_value = lax.dot_general(part_hidden, part_down, (((1,), (1,)), ((), ())), preferred_element_type=jnp.float32)
        rounded = lax.optimization_barrier(partial_value.astype(jnp.bfloat16))
        branch = branch + rounded.astype(jnp.float32)
    mixed = jnp.sqrt(jnp.float32(2.0)) * wide + 0.5 * branch
    center = lax.optimization_barrier(jnp.mean(mixed, axis=-1, keepdims=True))
    spread = lax.optimization_barrier(jnp.mean(jnp.square(mixed - center), axis=-1, keepdims=True))
    result = ((mixed - center) * lax.rsqrt(spread + 1e-05) * post_gain + post_bias).astype(jnp.bfloat16)
    return (gate_ready, up_ready, down_ready, result)
```

```python
import functools

import jax
import jax.numpy as jnp
from jax import lax
from jax.experimental import pallas as pl
from jax.experimental.pallas import tpu as pltpu
from jax.sharding import PartitionSpec as P

MESH = pl.DeviceIdType.MESH
LANES = 128


def finish(wide, branch, post_gain, post_bias):
    mixed = jnp.sqrt(jnp.float32(2.0)) * wide + 0.5 * branch
    center = jnp.mean(mixed, axis=-1, keepdims=True)
    spread = jnp.mean(jnp.square(mixed - center), axis=-1, keepdims=True)
    return ((mixed - center) * lax.rsqrt(spread + 1e-05) * post_gain + post_bias).astype(
        jnp.bfloat16
    )


def plain(tokens, gate_master, up_master, down_master, norm_gain, post_gain, post_bias):
    row_count = gate_master.shape[0]
    first_row = lax.axis_index("fs") * row_count
    gain_rows = lax.dynamic_slice_in_dim(norm_gain, first_row, row_count, 0)
    gate_piece = (gain_rows[:, None] * gate_master).astype(jnp.bfloat16)
    up_piece = (gain_rows[:, None] * up_master).astype(jnp.bfloat16)
    down_piece = down_master.astype(jnp.bfloat16)
    gate_ready, up_ready, down_ready = (
        lax.all_gather(gate_piece, "fs", axis=0, tiled=True),
        lax.all_gather(up_piece, "fs", axis=0, tiled=True),
        lax.all_gather(down_piece, "fs", axis=0, tiled=True),
    )
    wide = tokens.astype(jnp.float32)
    normed = (wide * lax.rsqrt(jnp.mean(wide * wide, axis=-1, keepdims=True) + 1e-06)).astype(
        jnp.bfloat16
    )
    piece = lax.all_gather(normed, "tp", axis=0, tiled=True)
    gate = jnp.dot(piece, gate_ready, preferred_element_type=jnp.float32)
    upward = jnp.dot(piece, up_ready, preferred_element_type=jnp.float32)
    hidden = (jax.nn.silu(gate) * upward).astype(jnp.bfloat16)
    branch = lax.psum_scatter(
        lax.dot_general(
            hidden, down_ready, (((1,), (1,)), ((), ())), preferred_element_type=jnp.float32
        ).astype(jnp.bfloat16),
        "tp",
        scatter_dimension=0,
        tiled=True,
    ).astype(jnp.float32)
    result = finish(wide, branch, post_gain, post_bias)
    return (gate_ready, up_ready, down_ready, result)


def fused_kernel(
    fs, tp, n, tok_ref, gm_ref, um_ref, dm_ref, gain_ref, pg_ref, pb_ref,
    go_ref, uo_ref, do_ref, res_ref,
    wire, fg, fu, fd, toks, hid, parts, got, mixed,
    up_sem, dn_sem, y_sem, r_sem, ts_sem, tr_sem, ps_sem, pr_sem, o_sem,
):
    y, z, t = lax.axis_index("grp"), lax.axis_index("fs"), lax.axis_index("tp")
    rc, cols = gm_ref.shape
    r = rc // (2 * n)
    q, tail = cols // LANES, cols % LANES
    half = LANES // 2
    tok_rows, d = tok_ref.shape
    up_dev = (y, jnp.minimum(z + 1, fs - 1), t)
    dn_dev = (y, jnp.maximum(z - 1, 0), t)
    y_dev = (1 - y, z, t)
    has_up, has_dn = z < fs - 1, z > 0
    full = (fg, fu, fd)
    outs = (go_ref, uo_ref, do_ref)
    masters = (gm_ref, um_ref, dm_ref)

    barrier = pltpu.get_barrier_semaphore()

    def greet(dev):
        pl.semaphore_signal(barrier, inc=1, device_id=dev, device_id_type=MESH)

    pl.when(has_up)(lambda: greet(up_dev))
    pl.when(has_dn)(lambda: greet(dn_dev))
    greet(y_dev)
    peers = [lax.rem(t + j, tp) for j in range(1, tp)]
    for peer in peers:
        greet((y, z, peer))

    def slot(m, b, h, c):
        return ((m * fs + b) * 2 + h) * n + c

    def hop(s, dev, sem):
        return pltpu.make_async_remote_copy(
            src_ref=wire.at[s], dst_ref=wire.at[s], send_sem=sem.at[s], recv_sem=r_sem.at[s],
            device_id=dev, device_id_type=MESH,
        )

    def row_of(b, h, c):
        return pl.multiple_of(b * rc + (h * n + c) * r, r)

    def put_out(m, row, count):
        pltpu.make_async_copy(
            full[m].at[pl.ds(row, count)], outs[m].at[pl.ds(row, count)], o_sem.at[m]
        ).start()

    def rounded(m, h, c):
        at = pl.ds(pl.multiple_of((h * n + c) * r, r), r)
        v = masters[m][at, :]
        if m < 2:
            v = v * gain_ref[at, :]
        return v.astype(jnp.bfloat16)

    def pack(m, c):
        v = rounded(m, y, c)
        row = row_of(z, y, c)
        full[m][pl.ds(row, r), :] = v
        s = slot(m, z, y, c)
        for k in range(q):
            wire[s, k * r:(k + 1) * r, :] = v[:, k * LANES:(k + 1) * LANES]
        if tail:
            e = v[:, q * LANES:].astype(jnp.float32)
            gap = jnp.zeros((r // 2, half - tail), jnp.float32)
            both = [e[:r // 2], gap, e[r // 2:], gap]
            wire[s, q * r:, :] = jnp.concatenate(both, axis=1).astype(jnp.bfloat16)

    def send_own(m, c):
        s = slot(m, z, y, c)
        pl.when(has_up)(lambda: hop(s, up_dev, up_sem).start())
        pl.when(has_dn)(lambda: hop(s, dn_dev, dn_sem).start())

    def keep_other(m, c):
        row = row_of(z, 1 - y, c)
        full[m][pl.ds(row, r), :] = rounded(m, 1 - y, c)

    def unpack(m, b, h, c):
        s, row = slot(m, b, h, c), row_of(b, h, c)
        for k in range(q):
            full[m][pl.ds(row, r), k * LANES:(k + 1) * LANES] = wire[s, k * r:(k + 1) * r, :]
        if tail:
            e = wire[s, q * r:, :].astype(jnp.float32)
            full[m][pl.ds(row, r // 2), q * LANES:] = e[:, :tail].astype(jnp.bfloat16)
            shifted = pltpu.roll(e, half, 1)
            at = pl.ds(pl.multiple_of(row + r // 2, r // 2), r // 2)
            full[m][at, q * LANES:] = shifted[:, :tail].astype(jnp.bfloat16)
        put_out(m, row, r)

    def down_rows(row):
        k = row // r
        w = fd[pl.ds(row, r), :]
        part = lax.dot_general(
            hid[...], w, (((1,), (1,)), ((), ())), preferred_element_type=jnp.float32
        )
        parts[k] = part.astype(jnp.bfloat16)
        for j, peer in enumerate(peers):
            part_copy(k, j, peer).start()

    def part_copy(k, j, peer):
        return pltpu.make_async_remote_copy(
            src_ref=parts.at[k, pl.ds(pl.multiple_of(peer * tok_rows, tok_rows), tok_rows)],
            dst_ref=got.at[t, k],
            send_sem=ps_sem.at[j, k], recv_sem=pr_sem.at[t, k],
            device_id=(y, z, peer), device_id_type=MESH,
        )

    def arrived(m, c, p, after):
        low, high = z - 1 - p, z + 1 + p

        @pl.when(low >= 0)
        def _():
            s = slot(m, low, y, c)
            hop(s, up_dev, up_sem).wait_recv()
            pl.when(has_up)(lambda: hop(s, up_dev, up_sem).start())
            hop(s, y_dev, y_sem).start()

        @pl.when(high <= fs - 1)
        def _():
            s = slot(m, high, y, c)
            hop(s, dn_dev, dn_sem).wait_recv()
            pl.when(has_dn)(lambda: hop(s, dn_dev, dn_sem).start())
            hop(s, y_dev, y_sem).start()

        for b, ok in ((low, low >= 0), (high, high <= fs - 1)):
            @pl.when(ok)
            def _(b=b):
                unpack(m, b, y, c)
                if after:
                    down_rows(row_of(b, y, c))

    def crossed(m, c, p, after):
        low, high = z - 1 - p, z + 1 + p
        for b, ok in ((low, low >= 0), (high, high <= fs - 1)):
            @pl.when(ok)
            def _(b=b):
                hop(slot(m, b, 1 - y, c), y_dev, y_sem).wait_recv()
                unpack(m, b, 1 - y, c)
                if after:
                    down_rows(row_of(b, 1 - y, c))

    first = [(m, c) for c in range(n) for m in (0, 1)]
    second = [(2, c) for c in range(n)]

    pack(*first[0])
    wide = tok_ref[...].astype(jnp.float32)
    scale = lax.rsqrt(jnp.mean(wide * wide, axis=-1, keepdims=True) + 1e-06)
    toks[t] = (wide * scale).astype(jnp.bfloat16)
    for pair in first[1:]:
        pack(*pair)
    expected = has_up.astype(jnp.int32) + has_dn.astype(jnp.int32) + tp
    pl.semaphore_wait(barrier, expected)
    for pair in first:
        send_own(*pair)

    def tok_copy(j, peer):
        return pltpu.make_async_remote_copy(
            src_ref=toks.at[t], dst_ref=toks.at[t],
            send_sem=ts_sem.at[j], recv_sem=tr_sem.at[t],
            device_id=(y, z, peer), device_id_type=MESH,
        )

    for j, peer in enumerate(peers):
        tok_copy(j, peer).start()
    for pair in second:
        pack(*pair)
    for pair in first + second:
        keep_other(*pair)
    for m in range(3):
        put_out(m, pl.multiple_of(z * rc, rc), rc)

    waiting = []
    for p in range(fs - 1):
        for m, c in first:
            arrived(m, c, p, False)
            waiting.append((m, c, p))
            if len(waiting) > 1:
                crossed(*waiting.pop(0), False)
    for pair in second:
        send_own(*pair)
    ready = False
    for p in range(fs - 1):
        for m, c in second:
            arrived(m, c, p, ready)
            waiting.append((m, c, p))
            if len(waiting) > 1:
                crossed(*waiting.pop(0), ready)
        if not ready:
            ready = True
            while waiting:
                crossed(*waiting.pop(0), False)
            for j, peer in enumerate(peers):
                pltpu.make_async_remote_copy(
                    src_ref=toks.at[peer], dst_ref=toks.at[peer],
                    send_sem=ts_sem.at[j], recv_sem=tr_sem.at[peer],
                    device_id=(y, z, peer), device_id_type=MESH,
                ).wait_recv()
            lhs = toks[...].reshape(tp * tok_rows, d)
            wide_step = 2 * LANES
            for lo in range(0, cols, wide_step):
                at = slice(lo, min(lo + wide_step, cols))
                gate = jnp.dot(lhs, fg[:, at], preferred_element_type=jnp.float32)
                upward = jnp.dot(lhs, fu[:, at], preferred_element_type=jnp.float32)
                hid[:, at] = (jax.nn.silu(gate) * upward).astype(jnp.bfloat16)
            for k in range(2 * n):
                down_rows(pl.multiple_of(z * rc + k * r, r))
            for c in range(n):
                for b, ok in ((z - 1, z - 1 >= 0), (z + 1, z + 1 <= fs - 1)):
                    @pl.when(ok)
                    def _(b=b, c=c):
                        down_rows(row_of(b, 0, c))
                        down_rows(row_of(b, 1, c))
    while waiting:
        crossed(*waiting.pop(0), True)

    chunks = d // r
    wide = tok_ref[...].astype(jnp.float32)
    mine = pl.ds(pl.multiple_of(t * tok_rows, tok_rows), tok_rows)
    for k in range(chunks):
        branch = parts[k, mine, :].astype(jnp.float32)
        for j, peer in enumerate(peers):
            pltpu.make_async_remote_copy(
                src_ref=got.at[peer, k], dst_ref=got.at[peer, k],
                send_sem=ps_sem.at[j, k], recv_sem=pr_sem.at[peer, k],
                device_id=(y, z, peer), device_id_type=MESH,
            ).wait_recv()
            branch = branch + got[peer, k].astype(jnp.float32)
        at = slice(k * r, (k + 1) * r)
        mixed[:, at] = jnp.sqrt(jnp.float32(2.0)) * wide[:, at] + 0.5 * branch
    mix = mixed[...]
    center = jnp.mean(mix, axis=-1, keepdims=True)
    off = mix - center
    spread = jnp.mean(jnp.square(off), axis=-1, keepdims=True)
    res_ref[...] = (
        off * lax.rsqrt(spread + 1e-05) * pg_ref[...] + pb_ref[...]
    ).astype(jnp.bfloat16)

    for m in range(3):
        pltpu.make_async_copy(full[m], outs[m], o_sem.at[m]).wait()
    for j, peer in enumerate(peers):
        tok_copy(j, peer).wait_send()
        for k in range(chunks):
            part_copy(k, j, peer).wait_send()
    for m in range(3):
        for c in range(n):
            for b in range(fs):
                s = slot(m, b, y, c)
                pl.when(has_up & (b <= z))(lambda s=s: hop(s, up_dev, up_sem).wait_send())
                pl.when(has_dn & (b >= z))(lambda s=s: hop(s, dn_dev, dn_sem).wait_send())
                pl.when(z != b)(lambda s=s: hop(s, y_dev, y_sem).wait_send())


def fused(fs, tp, n, tokens, gate_master, up_master, down_master, norm_gain, post_gain, post_bias):
    rc, cols = gate_master.shape
    tok_rows, d = tokens.shape
    r = rc // (2 * n)
    q, tail = cols // LANES, cols % LANES
    slots = 3 * fs * 2 * n
    first_row = lax.axis_index("fs") * rc
    gain_rows = lax.dynamic_slice_in_dim(norm_gain, first_row, rc, 0)[:, None]
    bf = jnp.bfloat16
    ready = jax.ShapeDtypeStruct((d, cols), bf)
    vmem = pl.BlockSpec(memory_space=pltpu.VMEM)
    anywhere = pl.BlockSpec(memory_space=pl.ANY)
    dma = pltpu.SemaphoreType.DMA
    return tuple(pl.pallas_call(
        functools.partial(fused_kernel, fs, tp, n),
        out_shape=(ready, ready, ready, jax.ShapeDtypeStruct((tok_rows, d), bf)),
        in_specs=[vmem] * 7,
        out_specs=(anywhere, anywhere, anywhere, vmem),
        scratch_shapes=[
            pltpu.VMEM((slots, q * r + (r // 2 if tail else 0), LANES), bf),
            pltpu.VMEM((d, cols), bf),
            pltpu.VMEM((d, cols), bf),
            pltpu.VMEM((d, cols), bf),
            pltpu.VMEM((tp, tok_rows, d), bf),
            pltpu.VMEM((tp * tok_rows, cols), bf),
            pltpu.VMEM((d // r, tp * tok_rows, r), bf),
            pltpu.VMEM((tp, d // r, tok_rows, r), bf),
            pltpu.VMEM((tok_rows, d), jnp.float32),
            dma((slots,)), dma((slots,)), dma((slots,)), dma((slots,)),
            dma((tp - 1,)), dma((tp,)),
            dma((tp - 1, d // r)), dma((tp, d // r)), dma((3,)),
        ],
        compiler_params=pltpu.CompilerParams(
            collective_id=0, has_side_effects=True, vmem_limit_bytes=60 * 2**20
        ),
    )(
        tokens, gate_master, up_master, down_master, gain_rows,
        post_gain[None, :], post_bias[None, :],
    ))


def solution(mesh):
    grp, fs, tp = mesh.shape["grp"], mesh.shape["fs"], mesh.shape["tp"]

    def local(tokens, gate_master, *rest):
        rc, cols = gate_master.shape
        n = rc // (2 * LANES)
        fits = grp == 2 and fs > 1 and rc % (2 * LANES) == 0 and 2 * n * fs <= 32
        fits = fits and cols % LANES <= LANES // 2 and tokens.shape[0] % 16 == 0
        if fits:
            return fused(fs, tp, n, tokens, gate_master, *rest)
        return plain(tokens, gate_master, *rest)

    return jax.shard_map(
        local,
        mesh=mesh,
        in_specs=(
            P(("grp", "fs", "tp"), None),
            P("fs", "tp"),
            P("fs", "tp"),
            P("fs", "tp"),
            P(),
            P(),
            P(),
        ),
        out_specs=(P("grp", "tp"), P("grp", "tp"), P("grp", "tp"), P(("grp", "fs", "tp"), None)),
        check_vma=False,
    )
```

```python
import functools

import jax
import jax.numpy as jnp
from jax import lax
from jax.experimental import pallas as pl
from jax.experimental.pallas import tpu as pltpu
from jax.sharding import PartitionSpec as P

MESH = pl.DeviceIdType.MESH
LANES = 128


def finish(wide, branch, post_gain, post_bias):
    mixed = jnp.sqrt(jnp.float32(2.0)) * wide + 0.5 * branch
    center = jnp.mean(mixed, axis=-1, keepdims=True)
    spread = jnp.mean(jnp.square(mixed - center), axis=-1, keepdims=True)
    return ((mixed - center) * lax.rsqrt(spread + 1e-05) * post_gain + post_bias).astype(
        jnp.bfloat16
    )


def plain(tokens, gate_master, up_master, down_master, norm_gain, post_gain, post_bias):
    row_count = gate_master.shape[0]
    first_row = lax.axis_index("fs") * row_count
    gain_rows = lax.dynamic_slice_in_dim(norm_gain, first_row, row_count, 0)
    gate_piece = (gain_rows[:, None] * gate_master).astype(jnp.bfloat16)
    up_piece = (gain_rows[:, None] * up_master).astype(jnp.bfloat16)
    down_piece = down_master.astype(jnp.bfloat16)
    gate_ready, up_ready, down_ready = (
        lax.all_gather(gate_piece, "fs", axis=0, tiled=True),
        lax.all_gather(up_piece, "fs", axis=0, tiled=True),
        lax.all_gather(down_piece, "fs", axis=0, tiled=True),
    )
    wide = tokens.astype(jnp.float32)
    normed = (wide * lax.rsqrt(jnp.mean(wide * wide, axis=-1, keepdims=True) + 1e-06)).astype(
        jnp.bfloat16
    )
    piece = lax.all_gather(normed, "tp", axis=0, tiled=True)
    gate = jnp.dot(piece, gate_ready, preferred_element_type=jnp.float32)
    upward = jnp.dot(piece, up_ready, preferred_element_type=jnp.float32)
    hidden = (jax.nn.silu(gate) * upward).astype(jnp.bfloat16)
    branch = lax.psum_scatter(
        lax.dot_general(
            hidden, down_ready, (((1,), (1,)), ((), ())), preferred_element_type=jnp.float32
        ).astype(jnp.bfloat16),
        "tp",
        scatter_dimension=0,
        tiled=True,
    ).astype(jnp.float32)
    result = finish(wide, branch, post_gain, post_bias)
    return (gate_ready, up_ready, down_ready, result)


def fused_kernel(
    fs, tp, n, tok_ref, gm_ref, um_ref, dm_ref, gain_ref, pg_ref, pb_ref,
    go_ref, uo_ref, do_ref, res_ref,
    stage, fg, fu, fd, toks, acc_g, acc_u, hid, parts, got, mixed,
    up_sem, dn_sem, y_sem, r_sem, ts_sem, tr_sem, ps_sem, pr_sem, o_sem, i_sem,
):
    y, z, t = lax.axis_index("grp"), lax.axis_index("fs"), lax.axis_index("tp")
    cols, rc = gm_ref.shape
    tok_rows, d = tok_ref.shape
    tiles = d // LANES
    full = (fg, fu, fd)
    outs = (go_ref, uo_ref, do_ref)
    masters = (gm_ref, um_ref, dm_ref)
    up_dev = (y, jnp.minimum(z + 1, fs - 1), t)
    dn_dev = (y, jnp.maximum(z - 1, 0), t)
    y_dev = (1 - y, z, t)
    has_up, has_dn = z < fs - 1, z > 0
    peers = [lax.rem(t + j, tp) for j in range(1, tp)]
    first = [(m, c) for m in (0, 1) for c in range(n)]
    second = [(2, c) for c in range(n)]

    def fetch(m, h, c):
        k = h * n + c
        return pltpu.make_async_copy(
            masters[m].at[:, pl.ds(pl.multiple_of(k * LANES, LANES), LANES)],
            stage.at[m, k], i_sem.at[m, k],
        )

    for h in (y, 1 - y):
        for m, c in first + second:
            fetch(m, h, c).start()

    barrier = pltpu.get_barrier_semaphore()

    def greet(dev):
        pl.semaphore_signal(barrier, inc=1, device_id=dev, device_id_type=MESH)

    pl.when(has_up)(lambda: greet(up_dev))
    pl.when(has_dn)(lambda: greet(dn_dev))
    greet(y_dev)
    for peer in peers:
        greet((y, z, peer))

    def tile_of(b, h, c):
        return b * (2 * n) + h * n + c

    def hop(m, k, dev, sem):
        s = m * tiles + k
        return pltpu.make_async_remote_copy(
            src_ref=full[m].at[k], dst_ref=full[m].at[k], send_sem=sem.at[s], recv_sem=r_sem.at[s],
            device_id=dev, device_id_type=MESH,
        )

    def put_out(m, k):
        pltpu.make_async_copy(
            full[m].at[k],
            outs[m].at[:, pl.ds(pl.multiple_of(k * LANES, LANES), LANES)],
            o_sem.at[m, k],
        ).start()

    def keep(m, h, c):
        fetch(m, h, c).wait()
        k = tile_of(z, h, c)
        v = stage[m, h * n + c]
        if m < 2:
            v = v * gain_ref[:, pl.ds(pl.multiple_of(k * LANES, LANES), LANES)]
        full[m][k] = v.astype(jnp.bfloat16)

    def send_own(m, c):
        k = tile_of(z, y, c)
        pl.when(has_up)(lambda: hop(m, k, up_dev, up_sem).start())
        pl.when(has_dn)(lambda: hop(m, k, dn_dev, dn_sem).start())

    def part_copy(k, j, peer):
        return pltpu.make_async_remote_copy(
            src_ref=parts.at[k, pl.ds(pl.multiple_of(peer * tok_rows, tok_rows), tok_rows)],
            dst_ref=got.at[t, k],
            send_sem=ps_sem.at[j, k], recv_sem=pr_sem.at[t, k],
            device_id=(y, z, peer), device_id_type=MESH,
        )

    def down_tile(k):
        part = jnp.dot(hid[...], fd[k], preferred_element_type=jnp.float32)
        parts[k] = part.astype(jnp.bfloat16)
        for j, peer in enumerate(peers):
            part_copy(k, j, peer).start()

    def add_tiles(m, k, start):
        acc = (acc_g, acc_u)[m]
        at = pl.ds(pl.multiple_of(k * LANES, LANES), n * LANES)
        lhs = toks[:, :, at].reshape(tp * tok_rows, n * LANES)
        rhs = jnp.concatenate([full[m][k + i] for i in range(n)], axis=1)
        term = lax.dot_general(
            lhs, rhs, (((1,), (1,)), ((), ())), preferred_element_type=jnp.float32
        )
        acc[...] = term if start else acc[...] + term

    def ends(p):
        low, high = z - 1 - p, z + 1 + p
        return ((low, low >= 0), (high, high <= fs - 1))

    sums, downs = [], []

    def later(m, b, ok, h, c):
        if m == 2:
            downs.append((ok, lambda: down_tile(tile_of(b, h, c))))
        elif c == n - 1:
            sums.append((ok, lambda: add_tiles(m, tile_of(b, h, 0), False)))

    def work(todo, count):
        for _ in range(min(count, len(todo))):
            ok, item = todo.pop(0)
            if ok is None:
                item()
            else:
                pl.when(ok)(item)

    def arrived(m, c, p):
        (low, has_low), (high, has_high) = ends(p)

        @pl.when(has_low)
        def _():
            k = tile_of(low, y, c)
            hop(m, k, up_dev, up_sem).wait_recv()
            hop(m, k, y_dev, y_sem).start()
            pl.when(has_up)(lambda: hop(m, k, up_dev, up_sem).start())
            put_out(m, k)

        @pl.when(has_high)
        def _():
            k = tile_of(high, y, c)
            hop(m, k, dn_dev, dn_sem).wait_recv()
            hop(m, k, y_dev, y_sem).start()
            pl.when(has_dn)(lambda: hop(m, k, dn_dev, dn_sem).start())
            put_out(m, k)

        for b, ok in ends(p):
            later(m, b, ok, y, c)

    def crossed(m, c, p):
        for b, ok in ends(p):
            @pl.when(ok)
            def _(b=b):
                k = tile_of(b, 1 - y, c)
                hop(m, k, y_dev, y_sem).wait_recv()
                put_out(m, k)
            later(m, b, ok, 1 - y, c)

    def tok_copy(j, peer, origin):
        return pltpu.make_async_remote_copy(
            src_ref=toks.at[origin], dst_ref=toks.at[origin],
            send_sem=ts_sem.at[j], recv_sem=tr_sem.at[origin],
            device_id=(y, z, peer), device_id_type=MESH,
        )

    wide = tok_ref[...].astype(jnp.float32)
    scale = lax.rsqrt(jnp.mean(wide * wide, axis=-1, keepdims=True) + 1e-06)
    toks[t] = (wide * scale).astype(jnp.bfloat16)
    keep(first[0][0], y, first[0][1])
    expected = has_up.astype(jnp.int32) + has_dn.astype(jnp.int32) + tp
    pl.semaphore_wait(barrier, expected)
    for before, pair in zip(first, first[1:]):
        keep(pair[0], y, pair[1])
        send_own(*before)
    for m, c in second:
        keep(m, y, c)
    send_own(*first[-1])
    for j, peer in enumerate(peers):
        tok_copy(j, peer, t).start()
    for m, c in first + second:
        keep(m, 1 - y, c)
    for m, c in first + second:
        for h in range(2):
            put_out(m, tile_of(z, h, c))

    waiting = []
    for p in range(fs - 1):
        for m, c in first:
            arrived(m, c, p)
            waiting.append((m, c, p))
            if len(waiting) > 1:
                crossed(*waiting.pop(0))
            if p > 0:
                work(sums, 4)
        if p == 0:
            for j, peer in enumerate(peers):
                tok_copy(j, peer, peer).wait_recv()
            own = [
                (None, lambda m=m, h=h: add_tiles(m, tile_of(z, h, 0), h == 0))
                for m in (0, 1) for h in (0, 1)
            ]
            sums[:0] = own
    for pair in second:
        send_own(*pair)
    for p in range(fs - 1):
        for m, c in second:
            arrived(m, c, p)
            waiting.append((m, c, p))
            if len(waiting) > 1:
                crossed(*waiting.pop(0))
            work(downs if p > 0 else sums, 4)
        if p == 0:
            work(sums, len(sums))
            hid[...] = (jax.nn.silu(acc_g[...]) * acc_u[...]).astype(jnp.bfloat16)
            downs[:0] = [
                (None, lambda h=h, c=c: down_tile(tile_of(z, h, c)))
                for h in (0, 1) for c in range(n)
            ]
    while waiting:
        crossed(*waiting.pop(0))
    work(downs, len(downs))

    wide = tok_ref[...].astype(jnp.float32)
    mine = pl.ds(pl.multiple_of(t * tok_rows, tok_rows), tok_rows)
    for k in range(tiles):
        branch = parts[k, mine, :].astype(jnp.float32)
        for j, peer in enumerate(peers):
            pltpu.make_async_remote_copy(
                src_ref=got.at[peer, k], dst_ref=got.at[peer, k],
                send_sem=ps_sem.at[j, k], recv_sem=pr_sem.at[peer, k],
                device_id=(y, z, peer), device_id_type=MESH,
            ).wait_recv()
            branch = branch + got[peer, k].astype(jnp.float32)
        at = slice(k * LANES, (k + 1) * LANES)
        mixed[:, at] = jnp.sqrt(jnp.float32(2.0)) * wide[:, at] + 0.5 * branch
    mix = mixed[...]
    center = jnp.mean(mix, axis=-1, keepdims=True)
    off = mix - center
    spread = jnp.mean(jnp.square(off), axis=-1, keepdims=True)
    res_ref[...] = (
        off * lax.rsqrt(spread + 1e-05) * pg_ref[...] + pb_ref[...]
    ).astype(jnp.bfloat16)

    for j, peer in enumerate(peers):
        tok_copy(j, peer, t).wait_send()
        for k in range(tiles):
            part_copy(k, j, peer).wait_send()
    for m in range(3):
        for k in range(tiles):
            pltpu.make_async_copy(
                full[m].at[k], outs[m].at[:, k * LANES:(k + 1) * LANES], o_sem.at[m, k]
            ).wait()
        for c in range(n):
            for b in range(fs):
                k = tile_of(b, y, c)
                pl.when(has_up & (b <= z))(lambda k=k: hop(m, k, up_dev, up_sem).wait_send())
                pl.when(has_dn & (b >= z))(lambda k=k: hop(m, k, dn_dev, dn_sem).wait_send())
                pl.when(z != b)(lambda k=k: hop(m, k, y_dev, y_sem).wait_send())


def fused(fs, tp, n, tokens, gate_master, up_master, down_master, norm_gain, post_gain, post_bias):
    rc, cols = gate_master.shape
    tok_rows, d = tokens.shape
    tiles, rows = d // LANES, tp * tok_rows
    bf, f32 = jnp.bfloat16, jnp.float32
    ready = jax.ShapeDtypeStruct((cols, d), bf)
    vmem = pl.BlockSpec(memory_space=pltpu.VMEM)
    anywhere = pl.BlockSpec(memory_space=pl.ANY)
    dma = pltpu.SemaphoreType.DMA
    gate, up, down, result = pl.pallas_call(
        functools.partial(fused_kernel, fs, tp, n),
        out_shape=(ready, ready, ready, jax.ShapeDtypeStruct((tok_rows, d), bf)),
        in_specs=[vmem] + [anywhere] * 3 + [vmem] * 3,
        out_specs=(anywhere, anywhere, anywhere, vmem),
        scratch_shapes=[
            pltpu.VMEM((3, 2 * n, cols, LANES), f32),
            pltpu.VMEM((tiles, cols, LANES), bf),
            pltpu.VMEM((tiles, cols, LANES), bf),
            pltpu.VMEM((tiles, cols, LANES), bf),
            pltpu.VMEM((tp, tok_rows, d), bf),
            pltpu.VMEM((rows, cols), f32),
            pltpu.VMEM((rows, cols), f32),
            pltpu.VMEM((rows, cols), bf),
            pltpu.VMEM((tiles, rows, LANES), bf),
            pltpu.VMEM((tp, tiles, tok_rows, LANES), bf),
            pltpu.VMEM((tok_rows, d), f32),
            dma((3 * tiles,)), dma((3 * tiles,)), dma((3 * tiles,)), dma((3 * tiles,)),
            dma((tp - 1,)), dma((tp,)),
            dma((tp - 1, tiles)), dma((tp, tiles)), dma((3, tiles)), dma((3, 2 * n)),
        ],
        compiler_params=pltpu.CompilerParams(
            collective_id=0, has_side_effects=True, vmem_limit_bytes=60 * 2**20
        ),
    )(
        tokens, gate_master.T, up_master.T, down_master.T, norm_gain[None, :],
        post_gain[None, :], post_bias[None, :],
    )
    return gate.T, up.T, down.T, result


def solution(mesh):
    grp, fs, tp = mesh.shape["grp"], mesh.shape["fs"], mesh.shape["tp"]

    def local(tokens, gate_master, *rest):
        rc, cols = gate_master.shape
        n = rc // (2 * LANES)
        fits = grp == 2 and fs > 1 and rc % (2 * LANES) == 0 and 2 * n * fs <= 32
        fits = fits and cols % 16 == 0 and tokens.shape[0] % 16 == 0
        if fits:
            return fused(fs, tp, n, tokens, gate_master, *rest)
        return plain(tokens, gate_master, *rest)

    return jax.shard_map(
        local,
        mesh=mesh,
        in_specs=(
            P(("grp", "fs", "tp"), None),
            P("fs", "tp"),
            P("fs", "tp"),
            P("fs", "tp"),
            P(),
            P(),
            P(),
        ),
        out_specs=(P("grp", "tp"), P("grp", "tp"), P("grp", "tp"), P(("grp", "fs", "tp"), None)),
        check_vma=False,
    )
```

```python
import functools

import jax
import jax.numpy as jnp
from jax import lax
from jax.experimental import pallas as pl
from jax.experimental.pallas import tpu as pltpu
from jax.sharding import PartitionSpec as P

MESH = pl.DeviceIdType.MESH
LANES = 128


def finish(wide, branch, post_gain, post_bias):
    mixed = jnp.sqrt(jnp.float32(2.0)) * wide + 0.5 * branch
    center = jnp.mean(mixed, axis=-1, keepdims=True)
    spread = jnp.mean(jnp.square(mixed - center), axis=-1, keepdims=True)
    return ((mixed - center) * lax.rsqrt(spread + 1e-05) * post_gain + post_bias).astype(
        jnp.bfloat16
    )


def plain(tokens, gate_master, up_master, down_master, norm_gain, post_gain, post_bias):
    row_count = gate_master.shape[0]
    first_row = lax.axis_index("fs") * row_count
    gain_rows = lax.dynamic_slice_in_dim(norm_gain, first_row, row_count, 0)
    gate_piece = (gain_rows[:, None] * gate_master).astype(jnp.bfloat16)
    up_piece = (gain_rows[:, None] * up_master).astype(jnp.bfloat16)
    down_piece = down_master.astype(jnp.bfloat16)
    gate_ready, up_ready, down_ready = (
        lax.all_gather(gate_piece, "fs", axis=0, tiled=True),
        lax.all_gather(up_piece, "fs", axis=0, tiled=True),
        lax.all_gather(down_piece, "fs", axis=0, tiled=True),
    )
    wide = tokens.astype(jnp.float32)
    normed = (wide * lax.rsqrt(jnp.mean(wide * wide, axis=-1, keepdims=True) + 1e-06)).astype(
        jnp.bfloat16
    )
    piece = lax.all_gather(normed, "tp", axis=0, tiled=True)
    gate = jnp.dot(piece, gate_ready, preferred_element_type=jnp.float32)
    upward = jnp.dot(piece, up_ready, preferred_element_type=jnp.float32)
    hidden = (jax.nn.silu(gate) * upward).astype(jnp.bfloat16)
    branch = lax.psum_scatter(
        lax.dot_general(
            hidden, down_ready, (((1,), (1,)), ((), ())), preferred_element_type=jnp.float32
        ).astype(jnp.bfloat16),
        "tp",
        scatter_dimension=0,
        tiled=True,
    ).astype(jnp.float32)
    result = finish(wide, branch, post_gain, post_bias)
    return (gate_ready, up_ready, down_ready, result)


def fused_kernel(
    fs, tp, n, tok_ref, gm_ref, um_ref, dm_ref, gain_ref, pg_ref, pb_ref,
    go_ref, uo_ref, do_ref, res_ref,
    stage, fg, fu, fd, toks, acc_g, acc_u, hid, parts, got, mixed,
    up_sem, dn_sem, y_sem, r_sem, ts_sem, tr_sem, ps_sem, pr_sem, o_sem, i_sem,
):
    y, z, t = lax.axis_index("grp"), lax.axis_index("fs"), lax.axis_index("tp")
    cols, rc = gm_ref.shape
    tok_rows, d = tok_ref.shape
    tiles = d // LANES
    full = (fg, fu, fd)
    outs = (go_ref, uo_ref, do_ref)
    masters = (gm_ref, um_ref, dm_ref)
    up_dev = (y, jnp.minimum(z + 1, fs - 1), t)
    dn_dev = (y, jnp.maximum(z - 1, 0), t)
    y_dev = (1 - y, z, t)
    has_up, has_dn = z < fs - 1, z > 0
    peers = [lax.rem(t + j, tp) for j in range(1, tp)]
    first = [(m, c) for m in (0, 1) for c in range(n)]
    second = [(2, c) for c in range(n)]

    def fetch(m, h, c):
        k = h * n + c
        return pltpu.make_async_copy(
            masters[m].at[:, pl.ds(pl.multiple_of(k * LANES, LANES), LANES)],
            stage.at[m, k], i_sem.at[m, k],
        )

    for h in (y, 1 - y):
        for m, c in first + second:
            fetch(m, h, c).start()

    barrier = pltpu.get_barrier_semaphore()

    def greet(dev):
        pl.semaphore_signal(barrier, inc=1, device_id=dev, device_id_type=MESH)

    pl.when(has_up)(lambda: greet(up_dev))
    pl.when(has_dn)(lambda: greet(dn_dev))
    greet(y_dev)
    for peer in peers:
        greet((y, z, peer))

    def tile_of(b, h, c):
        return b * (2 * n) + h * n + c

    def hop(m, k, dev, sem):
        s = m * tiles + k
        return pltpu.make_async_remote_copy(
            src_ref=full[m].at[k], dst_ref=full[m].at[k], send_sem=sem.at[s], recv_sem=r_sem.at[s],
            device_id=dev, device_id_type=MESH,
        )

    def put_out(m, k):
        pltpu.make_async_copy(
            full[m].at[k],
            outs[m].at[:, pl.ds(pl.multiple_of(k * LANES, LANES), LANES)],
            o_sem.at[m, k],
        ).start()

    def keep(m, h, c):
        fetch(m, h, c).wait()
        k = tile_of(z, h, c)
        v = stage[m, h * n + c]
        if m < 2:
            v = v * gain_ref[:, pl.ds(pl.multiple_of(k * LANES, LANES), LANES)]
        full[m][k] = v.astype(jnp.bfloat16)

    def send_own(m, c):
        k = tile_of(z, y, c)
        pl.when(has_up)(lambda: hop(m, k, up_dev, up_sem).start())
        pl.when(has_dn)(lambda: hop(m, k, dn_dev, dn_sem).start())

    def part_copy(k, j, peer):
        return pltpu.make_async_remote_copy(
            src_ref=parts.at[k, pl.ds(pl.multiple_of(peer * tok_rows, tok_rows), tok_rows)],
            dst_ref=got.at[t, k],
            send_sem=ps_sem.at[j, k], recv_sem=pr_sem.at[t, k],
            device_id=(y, z, peer), device_id_type=MESH,
        )

    def down_tile(k):
        part = jnp.dot(hid[...], fd[k], preferred_element_type=jnp.float32)
        parts[k] = part.astype(jnp.bfloat16)
        for j, peer in enumerate(peers):
            part_copy(k, j, peer).start()

    def add_tiles(m, k, start):
        acc = (acc_g, acc_u)[m]
        at = pl.ds(pl.multiple_of(k * LANES, LANES), n * LANES)
        lhs = toks[:, :, at].reshape(tp * tok_rows, n * LANES)
        rhs = jnp.concatenate([full[m][k + i] for i in range(n)], axis=1)
        term = lax.dot_general(
            lhs, rhs, (((1,), (1,)), ((), ())), preferred_element_type=jnp.float32
        )
        acc[...] = term if start else acc[...] + term

    def ends(p):
        low, high = z - 1 - p, z + 1 + p
        return ((low, low >= 0), (high, high <= fs - 1))

    sums, downs = [], []

    def later(m, b, ok, h, c):
        if m == 2:
            downs.append((ok, lambda: down_tile(tile_of(b, h, c))))
        elif c == n - 1:
            sums.append((ok, lambda: add_tiles(m, tile_of(b, h, 0), False)))

    def work(todo, count):
        for _ in range(min(count, len(todo))):
            ok, item = todo.pop(0)
            if ok is None:
                item()
            else:
                pl.when(ok)(item)

    def arrived(m, c, p):
        (low, has_low), (high, has_high) = ends(p)

        @pl.when(has_low)
        def _():
            k = tile_of(low, y, c)
            hop(m, k, up_dev, up_sem).wait_recv()
            hop(m, k, y_dev, y_sem).start()
            pl.when(has_up)(lambda: hop(m, k, up_dev, up_sem).start())
            put_out(m, k)

        @pl.when(has_high)
        def _():
            k = tile_of(high, y, c)
            hop(m, k, dn_dev, dn_sem).wait_recv()
            hop(m, k, y_dev, y_sem).start()
            pl.when(has_dn)(lambda: hop(m, k, dn_dev, dn_sem).start())
            put_out(m, k)

        for b, ok in ends(p):
            later(m, b, ok, y, c)

    def crossed(m, c, p):
        for b, ok in ends(p):
            @pl.when(ok)
            def _(b=b):
                k = tile_of(b, 1 - y, c)
                hop(m, k, y_dev, y_sem).wait_recv()
                put_out(m, k)
            later(m, b, ok, 1 - y, c)

    def tok_copy(j, peer, origin):
        return pltpu.make_async_remote_copy(
            src_ref=toks.at[origin], dst_ref=toks.at[origin],
            send_sem=ts_sem.at[j], recv_sem=tr_sem.at[origin],
            device_id=(y, z, peer), device_id_type=MESH,
        )

    wide = tok_ref[...].astype(jnp.float32)
    scale = lax.rsqrt(jnp.mean(wide * wide, axis=-1, keepdims=True) + 1e-06)
    toks[t] = (wide * scale).astype(jnp.bfloat16)
    keep(first[0][0], y, first[0][1])
    expected = has_up.astype(jnp.int32) + has_dn.astype(jnp.int32) + tp
    pl.semaphore_wait(barrier, expected)
    for before, pair in zip(first, first[1:]):
        keep(pair[0], y, pair[1])
        send_own(*before)
    for m, c in second:
        keep(m, y, c)
    send_own(*first[-1])
    for j, peer in enumerate(peers):
        tok_copy(j, peer, t).start()
    for m, c in first + second:
        keep(m, 1 - y, c)
    for m, c in first + second:
        for h in range(2):
            put_out(m, tile_of(z, h, c))

    waiting = []
    for p in range(fs - 1):
        for m, c in first:
            arrived(m, c, p)
            waiting.append((m, c, p))
            if len(waiting) > 2 * len(first):
                crossed(*waiting.pop(0))
            if p > 0:
                work(sums, 4)
        if p == 0:
            for j, peer in enumerate(peers):
                tok_copy(j, peer, peer).wait_recv()
            own = [
                (None, lambda m=m, h=h: add_tiles(m, tile_of(z, h, 0), h == 0))
                for m in (0, 1) for h in (0, 1)
            ]
            sums[:0] = own
    for pair in second:
        send_own(*pair)
    for p in range(fs - 1):
        for m, c in second:
            arrived(m, c, p)
            waiting.append((m, c, p))
            if p > 0 and len(waiting) > 2:
                crossed(*waiting.pop(0))
            work(downs if p > 0 else sums, 4)
        if p == 0:
            while waiting[0][0] < 2:
                crossed(*waiting.pop(0))
            work(sums, len(sums))
            hid[...] = (jax.nn.silu(acc_g[...]) * acc_u[...]).astype(jnp.bfloat16)
            downs[:0] = [
                (None, lambda h=h, c=c: down_tile(tile_of(z, h, c)))
                for h in (0, 1) for c in range(n)
            ]
    while waiting:
        crossed(*waiting.pop(0))
    work(downs, len(downs))

    wide = tok_ref[...].astype(jnp.float32)
    mine = pl.ds(pl.multiple_of(t * tok_rows, tok_rows), tok_rows)
    for k in range(tiles):
        branch = parts[k, mine, :].astype(jnp.float32)
        for j, peer in enumerate(peers):
            pltpu.make_async_remote_copy(
                src_ref=got.at[peer, k], dst_ref=got.at[peer, k],
                send_sem=ps_sem.at[j, k], recv_sem=pr_sem.at[peer, k],
                device_id=(y, z, peer), device_id_type=MESH,
            ).wait_recv()
            branch = branch + got[peer, k].astype(jnp.float32)
        at = slice(k * LANES, (k + 1) * LANES)
        mixed[:, at] = jnp.sqrt(jnp.float32(2.0)) * wide[:, at] + 0.5 * branch
    mix = mixed[...]
    center = jnp.mean(mix, axis=-1, keepdims=True)
    off = mix - center
    spread = jnp.mean(jnp.square(off), axis=-1, keepdims=True)
    res_ref[...] = (
        off * lax.rsqrt(spread + 1e-05) * pg_ref[...] + pb_ref[...]
    ).astype(jnp.bfloat16)

    for j, peer in enumerate(peers):
        tok_copy(j, peer, t).wait_send()
        for k in range(tiles):
            part_copy(k, j, peer).wait_send()
    for m in range(3):
        for k in range(tiles):
            pltpu.make_async_copy(
                full[m].at[k], outs[m].at[:, k * LANES:(k + 1) * LANES], o_sem.at[m, k]
            ).wait()
        for c in range(n):
            for b in range(fs):
                k = tile_of(b, y, c)
                pl.when(has_up & (b <= z))(lambda k=k: hop(m, k, up_dev, up_sem).wait_send())
                pl.when(has_dn & (b >= z))(lambda k=k: hop(m, k, dn_dev, dn_sem).wait_send())
                pl.when(z != b)(lambda k=k: hop(m, k, y_dev, y_sem).wait_send())


def fused(fs, tp, n, tokens, gate_master, up_master, down_master, norm_gain, post_gain, post_bias):
    rc, cols = gate_master.shape
    tok_rows, d = tokens.shape
    tiles, rows = d // LANES, tp * tok_rows
    bf, f32 = jnp.bfloat16, jnp.float32
    ready = jax.ShapeDtypeStruct((cols, d), bf)
    vmem = pl.BlockSpec(memory_space=pltpu.VMEM)
    anywhere = pl.BlockSpec(memory_space=pl.ANY)
    dma = pltpu.SemaphoreType.DMA
    gate, up, down, result = pl.pallas_call(
        functools.partial(fused_kernel, fs, tp, n),
        out_shape=(ready, ready, ready, jax.ShapeDtypeStruct((tok_rows, d), bf)),
        in_specs=[vmem] + [anywhere] * 3 + [vmem] * 3,
        out_specs=(anywhere, anywhere, anywhere, vmem),
        scratch_shapes=[
            pltpu.VMEM((3, 2 * n, cols, LANES), f32),
            pltpu.VMEM((tiles, cols, LANES), bf),
            pltpu.VMEM((tiles, cols, LANES), bf),
            pltpu.VMEM((tiles, cols, LANES), bf),
            pltpu.VMEM((tp, tok_rows, d), bf),
            pltpu.VMEM((rows, cols), f32),
            pltpu.VMEM((rows, cols), f32),
            pltpu.VMEM((rows, cols), bf),
            pltpu.VMEM((tiles, rows, LANES), bf),
            pltpu.VMEM((tp, tiles, tok_rows, LANES), bf),
            pltpu.VMEM((tok_rows, d), f32),
            dma((3 * tiles,)), dma((3 * tiles,)), dma((3 * tiles,)), dma((3 * tiles,)),
            dma((tp - 1,)), dma((tp,)),
            dma((tp - 1, tiles)), dma((tp, tiles)), dma((3, tiles)), dma((3, 2 * n)),
        ],
        compiler_params=pltpu.CompilerParams(
            collective_id=0, has_side_effects=True, vmem_limit_bytes=60 * 2**20
        ),
    )(
        tokens, gate_master.T, up_master.T, down_master.T, norm_gain[None, :],
        post_gain[None, :], post_bias[None, :],
    )
    return gate.T, up.T, down.T, result


def solution(mesh):
    grp, fs, tp = mesh.shape["grp"], mesh.shape["fs"], mesh.shape["tp"]

    def local(tokens, gate_master, *rest):
        rc, cols = gate_master.shape
        n = rc // (2 * LANES)
        fits = grp == 2 and fs > 1 and rc % (2 * LANES) == 0 and 2 * n * fs <= 32
        fits = fits and cols % 16 == 0 and tokens.shape[0] % 16 == 0
        if fits:
            return fused(fs, tp, n, tokens, gate_master, *rest)
        return plain(tokens, gate_master, *rest)

    return jax.shard_map(
        local,
        mesh=mesh,
        in_specs=(
            P(("grp", "fs", "tp"), None),
            P("fs", "tp"),
            P("fs", "tp"),
            P("fs", "tp"),
            P(),
            P(),
            P(),
        ),
        out_specs=(P("grp", "tp"), P("grp", "tp"), P("grp", "tp"), P(("grp", "fs", "tp"), None)),
        check_vma=False,
    )
```
